256 devices in a mesh: sp: 64 (over z, x, core), tp: 4 (over y).
Axes of the slice: x: 4, y: 4, z: 8, core: 2. Of those that a mesh axis runs over, the one named last changes fastest.
Arguments:
- query_maps: bfloat16 [12288, 1024], P('sp', 'tp'), may hold values from -6 to 6
- key_maps: bfloat16 [12288, 512], P('sp', 'tp'), may hold values from -6 to 6
- value_rows: bfloat16 [12288, 512], P('sp', 'tp'), may hold values from -6 to 6
- mix_lambda: float32 [8], P('tp'), may hold values from 0.3 to 0.8
- head_gain: float32 [128], replicated, may hold values from 0.1 to 1.9
- out_weight: bfloat16 [1024, 2048], replicated, may hold values from -0.1875 to 0.1875
- residual: bfloat16 [12288, 2048], P(('sp', 'tp')), may hold values from -6 to 6
- norm_gain: float32 [2048], replicated, may hold values from 0.1 to 1.9
- routes: int32 [12288, 4], P('sp'), may hold values from 0 to 63, all different within a row; in each aligned block of 48 rows (0 to 47, 48 to 95, ...) at most 6 rows name the same one
- route_weight: float32 [12288, 4], P(('sp', 'tp')), may hold values from 0.3 to 1.5
- expert_gate: bfloat16 [64, 2048, 1024], P('sp', None, 'tp'), may hold values from -0.125 to 0.125
- expert_up: bfloat16 [64, 2048, 1024], P('sp', None, 'tp'), may hold values from -0.125 to 0.125
- expert_down: bfloat16 [64, 1024, 2048], P('sp', 'tp'), may hold values from -0.1875 to 0.1875
- shared_gate: bfloat16 [2048, 1024], P(None, 'tp'), may hold values from -0.125 to 0.125
- shared_up: bfloat16 [2048, 1024], P(None, 'tp'), may hold values from -0.125 to 0.125
- shared_down: bfloat16 [1024, 2048], P('tp'), may hold values from -0.1875 to 0.1875
Outputs:
- mixed: bfloat16 [12288, 2048], P(('sp', 'tp'))
The draws below stay inside these ranges and needn't reach their ends.
Inputs may be any that keep to these rules, and one draw needn't show every extreme that they name: `routes`: the 4 experts of a token are different. In each aligned block of 48 tokens (the tokens of one device after the attention) no expert is named more than 6 times, a bound that some expert reaches in some blocks.
All inputs are finite; a program needn't handle non-finite values.
Results may differ from the reference program's by a relative error of at most 0.018.
Values may be sent and summed in bfloat16 or wider, within the bound.
A program may use at most 128 MiB of HBM per device.

```python
import math
import jax
import jax.numpy as jnp
import numpy as np
from jax import lax

D = 2048
HEADS = 8
KV_HEADS = 4
HD = 64
VD = 128
EXPERTS = 64
EXP_FF = 1024
SH_FF = 1024
TOP_K = 4
SEQ = 12288
ROWS_DEV = 48
CAP = 6
N_TP = 4


def base_values(key, salt, shape):
    values = jnp.clip(1.3 * jax.random.normal(jax.random.fold_in(key, salt), shape, jnp.float32), -6.0, 6.0)
    return values


def draw_key_maps(key, part):
    values = base_values(key, 7010, (SEQ, KV_HEADS * 2 * HD))
    return values.astype(jnp.bfloat16)


def draw_query_maps(key, part):
    values = base_values(key, 7020, (SEQ, HEADS * 2 * HD))
    return values.astype(jnp.bfloat16)


def levels(own_key, extent, pieces, low, top_value):
    def one(dim, shards_of):
        heights = jax.random.uniform(jax.random.fold_in(jax.random.fold_in(own_key, 6), dim), (shards_of,), jnp.float32, low / len(pieces), top_value / len(pieces))
        return jnp.repeat(jnp.exp(heights), extent[dim] // shards_of).reshape((-1,) + (1,) * (len(extent) - dim - 1))

    factor_of = one(*pieces[0])
    for cut in pieces[1:]:
        factor_of = factor_of * one(*cut)
    return factor_of


def routed_block(own_key, own, number, rows, amount, top, bound, skew):
    sequence = jax.random.permutation(own_key, amount)
    packed, ordinary = shares(amount, rows * top, bound, skew, True), shares(amount, rows * top, bound, skew, False)
    places = jnp.arange(amount)

    def named(sizes, offset_by):
        used = int((sizes > 0).sum())
        fixed = max(1, used // 4)
        shifted = fixed + (places - fixed + offset_by * (used - fixed)) % max(1, amount - fixed)
        return jnp.zeros((amount,), jnp.int32).at[sequence[jnp.where(places < fixed, places, shifted)]].set(jnp.asarray(sizes, jnp.int32))

    sizes = jnp.where(number % 4 == 0, named(packed, number // 4), named(ordinary, number - number // 4 - 1))
    mixed = jax.random.permutation(jax.random.fold_in(own, 3), amount)
    giver, taker = mixed[0:amount // 2 * 2:2], mixed[1:amount // 2 * 2:2]
    room = jnp.minimum(sizes[giver] - 1, bound - sizes[taker]) // 2
    room = jnp.where((giver == sequence[0]) | (taker == sequence[0]) | (sizes[taker] == 0), 0, jnp.maximum(room, 0))
    shifted = jax.random.randint(jax.random.fold_in(own, 4), (amount // 2,), 0, 1 << 20) % (room + 1)
    sizes = sizes.at[giver].add(-shifted).at[taker].add(shifted)
    members = jnp.searchsorted(jnp.cumsum(sizes), jnp.arange(rows * top), side="right").astype(jnp.int32)
    grid = members.reshape(top, rows).T
    grid = grid[jax.random.permutation(jax.random.fold_in(own, 1), rows)]
    offset_by = jax.random.randint(jax.random.fold_in(own, 2), (rows, 1), 0, top)
    return jnp.take_along_axis(grid, (jnp.arange(top)[None, :] + offset_by) % top, axis=1)


def shares(count, total, most, lean, full):
    portions = [(1 << 20) // math.isqrt(standing ** lean) + 1 for standing in range(1, count + 1)]
    largest = most if full else min(most, max(-(-total // count), total * portions[0] // sum(portions)))
    least = 1 if total - largest >= count - 1 else 0
    holding, surplus = [largest] + [least] * (count - 1), total - largest - least * (count - 1)
    while surplus > 0:
        candidates = [i for i in range(1, count) if holding[i] < largest] or [i for i in range(1, count) if holding[i] < most]
        mass, left = sum([portions[i] for i in candidates]), surplus
        for i in candidates:
            more = min(most - holding[i], max(1, left * portions[i] // mass), surplus)
            holding[i] = holding[i] + more
            surplus = surplus - more
    return np.array(holding)


def bell_draw(key, dims, spread, reach, shards=(), held_as=jnp.bfloat16):
    result = jax.random.normal(key, dims, jnp.float32) * spread
    if len(shards) > 0:
        result = levels(key, dims, shards, -0.22, 0.18) * result
    return jnp.clip(result, min=-reach, max=reach).astype(held_as)


def setup_inputs(seed: int = 0) -> dict:
    arg_keys = jax.random.split(jax.random.key(seed), 17)
    query_maps = draw_query_maps(jax.random.fold_in(arg_keys[16], 71), 0)
    key_maps = draw_key_maps(jax.random.fold_in(arg_keys[16], 71), 0)
    value_rows = bell_draw(arg_keys[2], (SEQ, KV_HEADS * VD), 1.0, 6.0, ((0, 64), (1, 4)))
    mix_lambda = jnp.clip(0.3 + 0.5 * jax.random.uniform(arg_keys[3], (HEADS,), jnp.float32) ** levels(arg_keys[3], (HEADS,), ((0, 4),), -0.2, 0.2), 0.3, 0.8)
    head_gain = jnp.clip(1.0 + 0.18 * jax.random.normal(arg_keys[4], (VD,), jnp.float32), 0.1, 1.9)
    out_weight = bell_draw(arg_keys[5], (HEADS * VD, D), (HEADS * VD) ** -0.5, 0.1875)
    residual = bell_draw(arg_keys[6], (SEQ, D), 1.0, 6.0, ((0, 256),))
    norm_gain = jnp.clip(1.0 + 0.18 * jax.random.normal(arg_keys[7], (D,), jnp.float32), 0.1, 1.9)
    routes_keys = jax.random.split(jax.random.fold_in(arg_keys[8], 1), SEQ // ROWS_DEV)
    routes_turns = jax.random.permutation(jax.random.fold_in(arg_keys[8], 3), SEQ // ROWS_DEV)
    routes = jax.vmap(lambda own, number: routed_block(jax.random.fold_in(arg_keys[8], 2), own, number, ROWS_DEV, EXPERTS, TOP_K, CAP, 2))(routes_keys, routes_turns).reshape((SEQ, TOP_K))
    route_weight = jnp.clip(jnp.exp(math.log(1.5) - 1.60943787 * jax.random.uniform(arg_keys[9], (SEQ, TOP_K), jnp.float32) ** levels(arg_keys[9], (SEQ, TOP_K), ((0, 256),), -0.2, 0.2)), 0.3, 1.5)
    expert_gate = bell_draw(arg_keys[10], (EXPERTS, D, EXP_FF), D ** -0.5, 0.125, ((0, 64), (2, 4)))
    expert_up = bell_draw(arg_keys[11], (EXPERTS, D, EXP_FF), D ** -0.5, 0.125, ((0, 64), (2, 4)))
    expert_down = bell_draw(arg_keys[12], (EXPERTS, EXP_FF, D), EXP_FF ** -0.5, 0.1875, ((0, 64), (1, 4)))
    shared_gate = bell_draw(arg_keys[13], (D, SH_FF), D ** -0.5, 0.125, ((1, 4),))
    shared_up = bell_draw(arg_keys[14], (D, SH_FF), D ** -0.5, 0.125, ((1, 4),))
    shared_down = bell_draw(arg_keys[15], (SH_FF, D), SH_FF ** -0.5, 0.1875, ((0, 4),))
    return dict(query_maps=query_maps, key_maps=key_maps, value_rows=value_rows, mix_lambda=mix_lambda, head_gain=head_gain, out_weight=out_weight, residual=residual, norm_gain=norm_gain, routes=routes, route_weight=route_weight, expert_gate=expert_gate, expert_up=expert_up, expert_down=expert_down, shared_gate=shared_gate, shared_up=shared_up, shared_down=shared_down)


norm_eps = 1e-06

def slot_targets(block_routes):
    flat_routes = block_routes.reshape(-1)
    onehot = (flat_routes[:, None] == jnp.arange(EXPERTS, dtype=jnp.int32)[None, :]).astype(jnp.int32)
    earlier = jnp.cumsum(onehot, axis=0) - onehot
    return (flat_routes, lax.optimization_barrier(jnp.sum(earlier * onehot, axis=1)).astype(jnp.int32))

def grouped_feedforward(token_rows, gate_weight, up_weight, down_weight):
    gate_value = jnp.dot(token_rows, gate_weight, preferred_element_type=jnp.float32)
    up_value = jnp.dot(token_rows, up_weight, preferred_element_type=jnp.float32)
    hidden = (jax.nn.silu(gate_value) * up_value).astype(jnp.bfloat16)
    group_width = hidden.shape[1] // N_TP
    running = jnp.zeros((token_rows.shape[0], down_weight.shape[1]), jnp.float32)
    for group_index in range(N_TP):
        partial_sum = jnp.dot(hidden[:, group_index * group_width:(group_index + 1) * group_width], down_weight[group_index * group_width:(group_index + 1) * group_width], preferred_element_type=jnp.float32)
        running = running + lax.optimization_barrier(partial_sum.astype(jnp.bfloat16)).astype(jnp.float32)
    return running.astype(jnp.bfloat16)

def head_attention(query_maps, key_maps, value_rows, mix_lambda, head_gain, head_index):
    kv_index = head_index // (HEADS // KV_HEADS)
    head_query = lax.dynamic_slice_in_dim(query_maps, (head_index * 2 * HD).astype(jnp.int32), 2 * HD, 1)
    head_key = lax.dynamic_slice_in_dim(key_maps, (kv_index * 2 * HD).astype(jnp.int32), 2 * HD, 1)
    head_value = lax.dynamic_slice_in_dim(value_rows, (kv_index * VD).astype(jnp.int32), VD, 1)
    head_lambda = mix_lambda[head_index]
    score_scale = HD ** (-0.5)
    block_rows = math.gcd(SEQ, 512)
    query_blocks = head_query.reshape(SEQ // block_rows, block_rows, 2 * HD)

    def weighted(scores):
        row_max = lax.optimization_barrier(jnp.max(scores, axis=1, keepdims=True))
        exp_scores = jnp.exp(scores - row_max)
        row_total = lax.optimization_barrier(jnp.sum(exp_scores, axis=1, keepdims=True))
        return jnp.dot(exp_scores.astype(jnp.bfloat16), head_value, preferred_element_type=jnp.float32) / row_total

    def one_block(query_block):
        first_map = jnp.dot(query_block[:, :HD], head_key[:, :HD].T, preferred_element_type=jnp.float32) * score_scale
        second_map = jnp.dot(query_block[:, HD:], head_key[:, HD:].T, preferred_element_type=jnp.float32) * score_scale
        difference = weighted(first_map) - head_lambda * weighted(second_map)
        inverse_rms = lax.rsqrt(lax.optimization_barrier(jnp.mean(difference * difference, axis=1, keepdims=True)) + norm_eps)
        return (difference * inverse_rms * head_gain).astype(jnp.bfloat16)
    return lax.map(one_block, query_blocks).reshape(SEQ, VD)

def reference(query_maps, key_maps, value_rows, mix_lambda, head_gain, out_weight, residual, norm_gain, routes, route_weight, expert_gate, expert_up, expert_down, shared_gate, shared_up, shared_down):

    def per_head(head_index):
        return head_attention(query_maps, key_maps, value_rows, mix_lambda, head_gain, head_index)
    attended = lax.map(per_head, jnp.arange(HEADS, dtype=jnp.int32))
    attended = jnp.transpose(attended, (1, 0, 2)).reshape(SEQ, HEADS * VD)
    projected = jnp.dot(attended, out_weight, preferred_element_type=jnp.float32)
    stream = (residual.astype(jnp.float32) + projected).astype(jnp.bfloat16)
    stream_wide = stream.astype(jnp.float32)
    inverse_rms = lax.rsqrt(lax.optimization_barrier(jnp.mean(stream_wide * stream_wide, axis=1, keepdims=True)) + norm_eps)
    normed = (stream_wide * inverse_rms * norm_gain).astype(jnp.bfloat16)
    blocks = SEQ // ROWS_DEV
    flat_routes, slot_index = jax.vmap(slot_targets)(routes.reshape(blocks, ROWS_DEV, TOP_K))
    expert_row = jnp.arange(blocks, dtype=jnp.int32)[:, None] * CAP + slot_index
    assignment = jnp.arange(SEQ * TOP_K, dtype=jnp.int32).reshape(blocks, ROWS_DEV * TOP_K)
    holder = jnp.full((EXPERTS, blocks * CAP), SEQ * TOP_K, jnp.int32).at[flat_routes, expert_row].set(assignment)
    padded_tokens = jnp.concatenate([normed, jnp.zeros((1, D), jnp.bfloat16)], axis=0)
    padded_weights = jnp.concatenate([route_weight.reshape(-1), jnp.zeros((1,), jnp.float32)], axis=0)

    def expert_step(running, inputs):
        holder_row, gate_weight, up_weight, down_weight = inputs
        token_index = holder_row // TOP_K
        outputs = grouped_feedforward(padded_tokens[token_index], gate_weight, up_weight, down_weight)
        contribution = padded_weights[holder_row][:, None] * outputs.astype(jnp.float32)
        return (running.at[token_index].add(contribution), None)
    routed_total = lax.scan(expert_step, jnp.zeros((SEQ + 1, D), jnp.float32), (holder, expert_gate, expert_up, expert_down))[0]
    shared_out = grouped_feedforward(normed, shared_gate, shared_up, shared_down)
    return (stream_wide + shared_out.astype(jnp.float32) + routed_total[:SEQ]).astype(jnp.bfloat16)
```

```python
from functools import partial

import jax
import jax.numpy as jnp
from jax import lax
from jax.experimental import pallas as pl
from jax.experimental.pallas import tpu as pltpu
from jax.sharding import Mesh
from jax.sharding import PartitionSpec as P

Z, X, C, Y = "sp_0", "sp_1", "sp_2", "tp"
SP = (Z, X, C)
SP_TP = (Z, X, C, Y)
MESH_ID = pl.DeviceIdType.MESH

norm_eps = 1e-06
lowest_score = -1e30
LOG2E = 1.4426950408889634

RELATED = slice(1, 4)
UP = {0: 0, 1: 1, 2: 3, 3: 5, 4: 7}
DOWN = {0: 0, 1: 2, 2: 4, 3: 6, 4: 7}


def partner(axis, offset):
    size = lax.axis_size(axis)
    return {axis: lax.rem(lax.axis_index(axis) + (offset + size) % size, size)}


class Sends:
    def __init__(self, sems):
        self.sems, self.copies = sems, []

    def __call__(self, src, dst, recv_sem, device):
        place = len(self.copies)

        def copy():
            return pltpu.make_async_remote_copy(
                src_ref=view(src),
                dst_ref=view(dst),
                send_sem=self.sems.at[place],
                recv_sem=view(recv_sem),
                device_id=device,
                device_id_type=MESH_ID,
            )

        self.copies.append(copy)
        copy().start()

    def finish(self):
        for copy in self.copies:
            copy().wait_send()


def view(place):
    return place[0].at[place[1:]] if isinstance(place, tuple) else place


def arrived(place, sem):
    pltpu.make_async_copy(view(place), view(place), view(sem)).wait()


def greet(partners):
    barrier = pltpu.get_barrier_semaphore()
    for device in partners:
        pl.semaphore_signal(barrier, inc=1, device_id=device, device_id_type=MESH_ID)
    pl.semaphore_wait(barrier, len(partners))


def attention_kernel(
    q_ref, k_ref, v_ref, lam_ref, gain_ref, ow_hbm, res_ref, ng_ref,
    stream_ref, normed_ref,
    keys, vals, qb, top, acc, att, heads, ow,
    send_sems, k_sems, v_sems, ks_sems, vs_sems, h_sems, ow_sem,
):
    rows = q_ref.shape[0]
    hd = k_ref.shape[1] // 2
    vd = v_ref.shape[1]
    n_heads = q_ref.shape[1] // (2 * hd)
    y = lax.axis_index(Y)
    sibling = partner(C, 1)
    above, below = partner(Z, 1), partner(Z, -1)
    along = {d: partner(X, d) for d in (1, 2, 3)}
    columns = {d: partner(Y, d) for d in (1, 2, 3)}
    load_ow = pltpu.make_async_copy(ow_hbm, ow, ow_sem)
    load_ow.start()
    greet([sibling, above, below, *along.values(), *columns.values()])
    send = Sends(send_sems)

    def k_up(d, r, src):
        send(src, (keys, 0, UP[d + 1], r), (k_sems, UP[d + 1], r), above)

    def k_down(d, r, src):
        send(src, (keys, 0, DOWN[d + 1], r), (k_sems, DOWN[d + 1], r), below)

    def v_up(d, src):
        send(src, (vals, 0, UP[d + 1], 0), (v_sems, UP[d + 1], 0), above)

    def v_down(d, src):
        send(src, (vals, 0, DOWN[d + 1], 0), (v_sems, DOWN[d + 1], 0), below)

    def v_along(slot, src, steps):
        for d in steps:
            send(src, (vals, 0, slot, 4 - d), (v_sems, slot, 4 - d), along[d])

    def k_row(sign, d, r):
        slot = UP[d] if sign > 0 else DOWN[d]
        block = (keys, 0, slot, r)
        arrived(block, (k_sems, slot, r))
        if sign > 0 and (d < 3 or (d == 3 and r < 2)):
            k_up(d, r, block)
        if sign < 0 and (d < 3 or (d == 3 and r >= 2)):
            k_down(d, r, block)

    def k_round(d, r):
        if d < 4:
            k_row(1, d, r)
            k_row(-1, d, r)
        else:
            k_row(1 if r < 2 else -1, d, r)

    def v_round(d):
        block = (vals, 0, UP[d], 0)
        arrived(block, (v_sems, UP[d], 0))
        if d < 4:
            v_up(d, block)
        v_along(UP[d], block, (1, 3) if UP[d] in (3, 5) else (1, 3, 2))
        if d < 4:
            block = (vals, 0, DOWN[d], 0)
            arrived(block, (v_sems, DOWN[d], 0))
            if d < 3:
                v_down(d, block)
            v_along(DOWN[d], block, (1, 3) if DOWN[d] in (4, 6) else (1, 3, 2))

    def v_take(slot, r):
        arrived((vals, 0, slot, r), (v_sems, slot, r))

    def v_relay(d):
        slot = UP[d]
        v_take(slot, 3)
        send((vals, 0, slot, 3), (vals, 0, slot, 2), (v_sems, slot, 2), along[1])
        slot = DOWN[d]
        v_take(slot, 1)
        send((vals, 0, slot, 1), (vals, 0, slot, 2), (v_sems, slot, 2), along[3])
        v_take(UP[d], 1)
        v_take(DOWN[d], 3)

    def share(buf, sems, slot):
        send((buf, 0, slot), (buf, 1, slot), (sems, slot), sibling)

    def shared(slot):
        arrived((keys, 1, slot), (ks_sems, slot))
        arrived((vals, 1, slot), (vs_sems, slot))

    for d in (1, 3, 2):
        send(k_ref, (keys, 0, 0, 4 - d), (k_sems, 0, 4 - d), along[d])
    k_up(0, 0, k_ref)
    k_down(0, 0, k_ref)
    v_up(0, v_ref)
    v_down(0, v_ref)
    v_along(0, v_ref, (1, 3, 2))
    send(k_ref, (keys, 1, 0, 0), (ks_sems, 8), sibling)
    send(v_ref, (vals, 1, 0, 0), (vs_sems, 8), sibling)
    keys[0, 0, 0] = k_ref[...]
    vals[0, 0, 0] = v_ref[...]
    lane = lax.broadcasted_iota(jnp.int32, (rows, 2 * hd), 1)
    for h in range(n_heads):
        head = q_ref[:, h * 2 * hd : (h + 1) * 2 * hd]
        for i in range(2):
            kept = jnp.logical_and(lane >= i * hd, lane < (i + 1) * hd)
            qb[pl.ds((2 * h + i) * rows, rows), :] = jnp.where(kept, head, jnp.zeros_like(head))
    top[...] = jnp.full(top.shape, lowest_score, jnp.float32)
    acc[...] = jnp.zeros(acc.shape, jnp.float32)

    def event_0():
        for r in (1, 3, 2):
            block = (keys, 0, 0, r)
            arrived(block, (k_sems, 0, r))
            k_up(0, r, block)
            k_down(0, r, block)
        send((keys, 0, 0, RELATED), (keys, 1, 0, RELATED), (ks_sems, 0), sibling)
        for r in (1, 3, 2):
            v_take(0, r)
        send((vals, 0, 0, RELATED), (vals, 1, 0, RELATED), (vs_sems, 0), sibling)

    def event_1():
        v_round(1)
        k_round(1, 0)
        for buf, sems in ((keys, ks_sems), (vals, vs_sems)):
            arrived((buf, 1, 0, 0), (sems, 8))
            arrived((buf, 1, 0, RELATED), (sems, 0))

    def event_2():
        for r in (1, 3, 2):
            k_round(1, r)
        share(keys, ks_sems, 1)
        share(keys, ks_sems, 2)
        v_round(2)
        for slot in (1, 2):
            for r in (1, 3, 2):
                v_take(slot, r)
            share(vals, vs_sems, slot)

    def event_3():
        k_round(2, 0)

    def event_4():
        k_round(2, 1)
        v_round(3)
        v_relay(2)
        shared(1)

    def event_5():
        k_round(2, 3)
        shared(2)

    def event_6():
        k_round(2, 2)
        share(keys, ks_sems, 3)
        share(keys, ks_sems, 4)
        v_round(4)
        for slot in (3, 4):
            v_take(slot, 2)
            share(vals, vs_sems, slot)

    def event_7():
        k_round(3, 0)
        v_relay(3)

    def event_8():
        k_round(3, 1)
        shared(3)

    def event_9():
        k_round(3, 3)
        shared(4)

    def event_10():
        k_round(3, 2)
        share(keys, ks_sems, 5)
        share(keys, ks_sems, 6)
        for slot in (5, 6):
            v_take(slot, 2)
            share(vals, vs_sems, slot)

    def event_11():
        for r in (1, 3, 2):
            v_take(7, r)
        share(vals, vs_sems, 7)

    def event_12():
        shared(5)

    def event_13():
        shared(6)

    def event_14():
        for r in (0, 1, 3, 2):
            k_round(4, r)
        share(keys, ks_sems, 7)

    def event_15():
        shared(7)

    events = [
        event_0, event_1, event_2, event_3, event_4, event_5, event_6, event_7,
        event_8, event_9, event_10, event_11, event_12, event_13, event_14, event_15,
    ]
    block = rows * 4
    factor = LOG2E * hd**-0.5

    def step(t, carry):
        for number, event in enumerate(events):
            pl.when(t == number)(event)
        since = t - 2
        slot = jnp.where(t < 2, 0, jnp.where(t >= 14, 7, 1 + 2 * (since // 4) + since % 2))
        side = jnp.where(t < 2, t, jnp.where(t >= 14, t - 14, (since % 4) // 2))
        key_block = keys[side, slot].reshape(block, 2 * hd)
        value_block = vals[side, slot].reshape(block, vd)
        widened = jnp.concatenate([value_block, jnp.ones((block, vd), jnp.bfloat16)], axis=1)
        for b in range(2 * n_heads):
            at = pl.ds(b * rows, rows)
            scores = lax.dot_general(
                qb[at, :], key_block, (((1,), (1,)), ((), ())), preferred_element_type=jnp.float32
            )
            old_top = top[at, :]
            new_top = jnp.maximum(old_top, jnp.max(scores, axis=1, keepdims=True))
            top[at, :] = new_top
            rescale = jnp.exp2((old_top - new_top) * factor)
            weights = jnp.exp2((scores - jnp.tile(new_top, (1, block // vd))) * factor).astype(jnp.bfloat16)
            update = jnp.dot(weights, widened, preferred_element_type=jnp.float32)
            acc[at, :] = acc[at, :] * jnp.tile(rescale, (1, 2)) + update
        return carry

    lax.fori_loop(0, 16, step, 0)

    rows_dev = rows // 4
    for h in range(n_heads):
        first = acc[pl.ds(2 * h * rows, rows), :]
        second = acc[pl.ds((2 * h + 1) * rows, rows), :]
        difference = first[:, :vd] / first[:, vd:] - lam_ref[h] * (second[:, :vd] / second[:, vd:])
        square = jnp.mean(difference * difference, axis=1, keepdims=True)
        scaled = (difference * lax.rsqrt(square + norm_eps) * gain_ref[...]).astype(jnp.bfloat16)
        for j in range(4):
            att[j, :, h * vd : (h + 1) * vd] = scaled[j * rows_dev : (j + 1) * rows_dev]
    for d in (1, 3, 2):
        send((att, lax.rem(y + d, 4)), (heads, 4 - d), (h_sems, 4 - d), columns[d])
    load_ow.wait()
    width = n_heads * vd
    total = jnp.dot(
        att[y], ow[pl.ds(pl.multiple_of(y * width, width), width), :], preferred_element_type=jnp.float32
    )
    for r in (1, 3, 2):
        arrived((heads, r), (h_sems, r))
        start = pl.multiple_of(lax.rem(y + r, 4) * width, width)
        total = total + jnp.dot(heads[r], ow[pl.ds(start, width), :], preferred_element_type=jnp.float32)
    stream = (res_ref[...].astype(jnp.float32) + total).astype(jnp.bfloat16)
    stream_ref[...] = stream
    wide = stream.astype(jnp.float32)
    rms = lax.rsqrt(jnp.mean(wide * wide, axis=1, keepdims=True) + norm_eps)
    normed_ref[...] = (wide * rms * ng_ref[...]).astype(jnp.bfloat16)
    send.finish()


def attention(query_maps, key_maps, value_rows, mix_lambda, head_gain, out_weight, residual, norm_gain):
    rows = query_maps.shape[0]
    rows_dev, width = residual.shape
    vmem = pl.BlockSpec(memory_space=pltpu.VMEM)
    out = jax.ShapeDtypeStruct(residual.shape, jnp.bfloat16)
    kw = key_maps.shape[1]
    vd = value_rows.shape[1]
    blocks = 2 * query_maps.shape[1] // kw
    return pl.pallas_call(
        attention_kernel,
        out_shape=(out, out),
        in_specs=[
            vmem, vmem, vmem, pl.BlockSpec(memory_space=pltpu.SMEM), vmem,
            pl.BlockSpec(memory_space=pl.ANY), vmem, vmem,
        ],
        out_specs=(vmem, vmem),
        scratch_shapes=[
            pltpu.VMEM((2, 8, 4, rows, kw), jnp.bfloat16),
            pltpu.VMEM((2, 8, 4, rows, vd), jnp.bfloat16),
            pltpu.VMEM((blocks * rows, kw), jnp.bfloat16),
            pltpu.VMEM((blocks * rows, vd), jnp.float32),
            pltpu.VMEM((blocks * rows, 2 * vd), jnp.float32),
            pltpu.VMEM((4, rows_dev, query_maps.shape[1]), jnp.bfloat16),
            pltpu.VMEM((4, rows_dev, query_maps.shape[1]), jnp.bfloat16),
            pltpu.VMEM(out_weight.shape, jnp.bfloat16),
            pltpu.SemaphoreType.DMA((96,)),
            pltpu.SemaphoreType.DMA((8, 4)),
            pltpu.SemaphoreType.DMA((8, 4)),
            pltpu.SemaphoreType.DMA((9,)),
            pltpu.SemaphoreType.DMA((9,)),
            pltpu.SemaphoreType.DMA((4,)),
            pltpu.SemaphoreType.DMA,
        ],
        compiler_params=pltpu.CompilerParams(collective_id=0, has_side_effects=True, vmem_limit_bytes=40 << 20),
        cost_estimate=pl.CostEstimate(flops=4 * 10**9, bytes_accessed=8 << 20, transcendentals=10**7),
        name="attention",
    )(query_maps, key_maps, value_rows, mix_lambda, head_gain.reshape(1, -1), out_weight, residual, norm_gain.reshape(1, -1))


def in_order(pieces, dim):
    dims = list(pieces.shape[1:])
    dims[dim] *= pieces.shape[0]
    return jnp.moveaxis(pieces, 0, dim).reshape(dims)


def from_everyone(shard, axis):
    copies = jnp.broadcast_to(shard, (lax.axis_size(axis), *shard.shape))
    return lax.all_to_all(copies, axis, split_axis=0, concat_axis=0, tiled=True)


def collect(shard, axis, dim):
    pieces = from_everyone(shard, axis)
    return in_order(pieces, dim)


def slot_targets(block_routes, experts, capacity):
    flat_routes = block_routes.reshape(-1)
    onehot = (flat_routes[:, None] == jnp.arange(experts, dtype=jnp.int32)[None, :]).astype(
        jnp.int32
    )
    earlier = jnp.cumsum(onehot, axis=0) - onehot
    return flat_routes * capacity + jnp.sum(earlier * onehot, axis=1)


def build_buffer(token_rows, block_routes, experts, capacity):
    targets = slot_targets(block_routes, experts, capacity)
    row_total = block_routes.shape[0]
    route_count = block_routes.shape[1]
    source_row = jnp.arange(row_total * route_count, dtype=jnp.int32) // route_count
    holder = jnp.full((experts * capacity,), row_total, jnp.int32).at[targets].set(source_row)
    padded = jnp.concatenate(
        [token_rows, jnp.zeros((1, token_rows.shape[1]), token_rows.dtype)], axis=0
    )
    return (padded[holder], targets)


def whole_experts(arrived, gate, up, down, senders, capacity):
    width = arrived.shape[-1]
    rows_in = arrived.reshape(senders * capacity, width)
    gate_value = jnp.einsum("td,gdf->gtf", rows_in, gate[:, 0], preferred_element_type=jnp.float32)
    up_value = jnp.einsum("td,gdf->gtf", rows_in, up[:, 0], preferred_element_type=jnp.float32)
    hidden = (jax.nn.silu(gate_value) * up_value).astype(jnp.bfloat16)
    return jnp.einsum("gtf,gfd->td", hidden, down[:, 0], preferred_element_type=jnp.float32).astype(jnp.bfloat16)


def body(
    query_maps, key_maps, value_rows, mix_lambda, head_gain, out_weight, residual, norm_gain,
    routes, route_weight, expert_gate, expert_up, expert_down, shared_gate, shared_up, shared_down,
):
    whole_gate, whole_up, whole_down = (lax.all_gather(w, "tp") for w in (expert_gate, expert_up, expert_down))
    stream, normed = attention(
        query_maps, key_maps, value_rows, mix_lambda, head_gain, out_weight, residual, norm_gain
    )
    stream_wide = stream.astype(jnp.float32)
    column = lax.axis_index("tp")
    rows_dev = residual.shape[0]
    senders = lax.axis_size(SP)
    experts = senders
    route_count = routes.shape[1]
    capacity = max(2, 2 * rows_dev * route_count // experts)
    own_routes = lax.dynamic_slice_in_dim(routes, column * rows_dev, rows_dev, 0)
    buffer, targets = build_buffer(normed, own_routes, experts, capacity)
    arrived = lax.all_to_all(buffer, SP, split_axis=0, concat_axis=0, tiled=True)
    local_routed = whole_experts(arrived, whole_gate, whole_up, whole_down, senders, capacity)
    shared_rows = collect(normed[None], "tp", 0)
    shared_in = shared_rows
    shared_in = shared_in.reshape(1 * lax.axis_size("tp") * rows_dev, shared_in.shape[-1])
    shared_hidden = (
        jax.nn.silu(jnp.dot(shared_in, shared_gate, preferred_element_type=jnp.float32))
        * jnp.dot(shared_in, shared_up, preferred_element_type=jnp.float32)
    ).astype(jnp.bfloat16)
    shared_out = jnp.dot(shared_hidden, shared_down, preferred_element_type=jnp.float32)
    pieces = shared_out.reshape(1 * lax.axis_size("tp"), rows_dev, shared_out.shape[-1])
    terms_out = pieces.astype(jnp.bfloat16)
    summed = (
        lax.psum_scatter(
            lax.optimization_barrier(terms_out).astype(jnp.float32).astype(jnp.bfloat16),
            "tp",
            scatter_dimension=0,
            tiled=True,
        )
        .astype(jnp.float32)[0]
        .astype(jnp.bfloat16)
    )
    returned = lax.all_to_all(local_routed, SP, split_axis=0, concat_axis=0, tiled=True)
    picked = (
        returned[targets].reshape(rows_dev, route_count, returned.shape[-1]).astype(jnp.float32)
    )
    routed_sum = jnp.sum(route_weight[:, :, None] * picked, axis=1)
    return (stream_wide + summed.astype(jnp.float32) + routed_sum).astype(jnp.bfloat16)


def solution(mesh):
    split = Mesh(mesh.devices.reshape(8, 4, 2, mesh.shape["tp"]), ("sp_0", "sp_1", "sp_2", "tp"))
    return jax.shard_map(
        body,
        mesh=split,
        in_specs=(
            P(SP, "tp"),
            P(SP, "tp"),
            P(SP, "tp"),
            P("tp"),
            P(),
            P(),
            P(SP_TP, None),
            P(),
            P(SP, None),
            P(SP_TP, None),
            P(SP, None, "tp"),
            P(SP, None, "tp"),
            P(SP, "tp", None),
            P(None, "tp"),
            P(None, "tp"),
            P("tp", None),
        ),
        out_specs=P(SP_TP, None),
        check_vma=False,
    )
```
